256 devices in a mesh: sp: 32 (over z, y), tp: 8 (over x, core).
Axes of the slice: x: 4, y: 4, z: 8, core: 2. Of those that a mesh axis runs over, the one named last changes fastest.
Arguments:
- query_a: bfloat16 [6144, 2048], P('sp', 'tp'), may hold values from -7.5 to 7.5
- key_a: bfloat16 [6144, 1024], P('sp', 'tp'), may hold values from -7.5 to 7.5
- value_a: bfloat16 [6144, 1024], P('sp', 'tp'), may hold values from -6 to 6
- query_b: bfloat16 [6144, 2048], P('sp', 'tp'), may hold values from -7.5 to 7.5
- key_b: bfloat16 [6144, 512], P('sp', 'tp'), may hold values from -7.5 to 7.5
- value_b: bfloat16 [6144, 512], P('sp', 'tp'), may hold values from -6 to 6
- gain_a: float32 [2, 128], replicated, may hold values from 1 to 6.5
- gain_b: float32 [2, 64], replicated, may hold values from 1 to 8.5
- out_a: bfloat16 [2048, 4096], P('tp'), may hold values from -0.5 to 0.5
- out_b: bfloat16 [2048, 4096], P('tp'), may hold values from -0.5 to 0.5
- residual: bfloat16 [6144, 4096], P('sp'), may hold values from -6 to 6
- norm_gain: float32 [4096], replicated, may hold values from 0.1 to 1.9
- gate_weight: bfloat16 [4096, 6144], P('sp', 'tp'), may hold values from -0.09375 to 0.09375
- up_weight: bfloat16 [4096, 6144], P('sp', 'tp'), may hold values from -0.09375 to 0.09375
- down_weight: bfloat16 [6144, 4096], P('tp', 'sp'), may hold values from -0.3125 to 0.3125
Outputs:
- output: bfloat16 [6144, 4096], P(('sp', 'tp'))
The draws below stay inside these ranges and needn't reach their ends.
All inputs are finite; a program needn't handle non-finite values.
Results may differ from the reference program's by a relative error of at most 0.017.
The reference program's roundings to bfloat16 on the way count: a program that leaves them out, or rounds other values in their place, can miss the bound.
Values may be sent and summed in bfloat16 or wider, within the bound.
No kernel may reach another device: no remote copies, remote signals or barrier semaphores. Data moves between devices by JAX's collectives and lax.ppermute only.
A program may use at most 128 MiB of HBM per device.

```python
import math
import jax
import jax.numpy as jnp
from jax import lax

HEAD_A = 128
HEAD_B = 64
HEADS_A = 16
KV_A = 8
HEADS_B = 32
KV_B = 8
FF = 6144
GRID_W = 64
D = 4096
TOKENS = 6144
N_TP = 8


def plant_pairs(key, query_heads, kv_heads, head_size):
    keys_split = jax.random.split(key, 2)
    queries = jax.random.normal(keys_split[0], (TOKENS, query_heads * head_size), jnp.float32)
    key_rows = jax.random.normal(keys_split[1], (TOKENS, kv_heads * head_size), jnp.float32)
    return (jnp.clip(queries, -7.5, 7.5), jnp.clip(key_rows, -7.5, 7.5))


def draw_query_a(key, part):
    return plant_pairs(jax.random.fold_in(key, 11), HEADS_A, KV_A, HEAD_A)[0].astype(jnp.bfloat16)


def draw_key_a(key, part):
    return plant_pairs(jax.random.fold_in(key, 11), HEADS_A, KV_A, HEAD_A)[1].astype(jnp.bfloat16)


def draw_query_b(key, part):
    return plant_pairs(jax.random.fold_in(key, 12), HEADS_B, KV_B, HEAD_B)[0].astype(jnp.bfloat16)


def draw_key_b(key, part):
    return plant_pairs(jax.random.fold_in(key, 12), HEADS_B, KV_B, HEAD_B)[1].astype(jnp.bfloat16)


def draw_gain_a(key, part):
    return jax.random.uniform(jax.random.fold_in(key, 21), (2, HEAD_A), jnp.float32, 1.0, 2.0)


def draw_gain_b(key, part):
    return jax.random.uniform(jax.random.fold_in(key, 22), (2, HEAD_B), jnp.float32, 1.0, 2.0)


def block_scale(rng, shape, cuts, smallest, largest):
    def one(dim, shards_of):
        draws = jax.random.uniform(jax.random.fold_in(jax.random.fold_in(rng, 6), dim), (shards_of,), jnp.float32, smallest / len(cuts), largest / len(cuts))
        return jnp.repeat(jnp.exp(draws), shape[dim] // shards_of).reshape((-1,) + (1,) * (len(shape) - dim - 1))

    factor_of = one(*cuts[0])
    for cut in cuts[1:]:
        factor_of = factor_of * one(*cut)
    return factor_of


def bell_draw(stream_key, shape, width, bound, cuts=(), kind=jnp.bfloat16):
    values = jax.random.normal(stream_key, shape, jnp.float32) * width
    if len(cuts) > 0:
        values = block_scale(stream_key, shape, cuts, -0.22, 0.18) * values
    return jnp.clip(values, min=-bound, max=bound).astype(kind)


def setup_inputs(seed: int = 0) -> dict:
    key_list = jax.random.split(jax.random.key(seed), 16)
    return {
        "query_a": draw_query_a(jax.random.fold_in(key_list[15], 71), 0),
        "key_a": draw_key_a(jax.random.fold_in(key_list[15], 71), 0),
        "value_a": bell_draw(key_list[2], (TOKENS, KV_A * HEAD_A), 1.0, 6.0, ((0, 32), (1, 8))),
        "query_b": draw_query_b(jax.random.fold_in(key_list[15], 71), 0),
        "key_b": draw_key_b(jax.random.fold_in(key_list[15], 71), 0),
        "value_b": bell_draw(key_list[5], (TOKENS, KV_B * HEAD_B), 1.0, 6.0, ((0, 32), (1, 8))),
        "gain_a": draw_gain_a(jax.random.fold_in(key_list[15], 71), 0),
        "gain_b": draw_gain_b(jax.random.fold_in(key_list[15], 71), 0),
        "out_a": bell_draw(key_list[8], (HEADS_A * HEAD_A, D), (D // 25) ** -0.5, 0.5, ((0, 8),)),
        "out_b": bell_draw(key_list[9], (HEADS_B * HEAD_B, D), (D // 25) ** -0.5, 0.5, ((0, 8),)),
        "residual": bell_draw(key_list[10], (TOKENS, D), 1.0, 6.0, ((0, 32),)),
        "norm_gain": jnp.clip(1.0 + 0.18 * jax.random.normal(key_list[11], (D,), jnp.float32), 0.1, 1.9),
        "gate_weight": bell_draw(key_list[12], (D, FF), D ** -0.5, 0.09375, ((0, 32), (1, 8))),
        "up_weight": bell_draw(key_list[13], (D, FF), D ** -0.5, 0.09375, ((0, 32), (1, 8))),
        "down_weight": bell_draw(key_list[14], (FF, D), (FF // 16) ** -0.5, 0.3125, ((0, 8), (1, 32))),
    }


epsilon = 1e-06
theta_base = 10000.0

def rotate(inputs, num_heads, head_size, first_pos, gain):
    tok_rows = inputs.shape[0]
    vectors = inputs.astype(jnp.float32).reshape(tok_rows, num_heads, head_size)
    vectors = vectors * lax.rsqrt(lax.optimization_barrier(jnp.mean(vectors * vectors, axis=-1, keepdims=True)) + epsilon) * gain
    position = first_pos + jnp.arange(tok_rows, dtype=jnp.int32)
    grid_row = (position // GRID_W).astype(jnp.float32)
    grid_col = (position % GRID_W).astype(jnp.float32)
    quarter = head_size // 4
    inv_freq = theta_base ** (-4.0 * jnp.arange(quarter, dtype=jnp.float32) / head_size)
    angle_row = grid_row[:, None] * inv_freq[None, :]
    angle_col = grid_col[:, None] * inv_freq[None, :]
    angles = jnp.concatenate([angle_row, angle_row, angle_col, angle_col], axis=-1)
    quarters = vectors.reshape(tok_rows, num_heads, 4, quarter)
    rotated = jnp.stack([-quarters[:, :, 1], quarters[:, :, 0], -quarters[:, :, 3], quarters[:, :, 2]], axis=2)
    rotated = rotated.reshape(tok_rows, num_heads, head_size)
    result = vectors * jnp.cos(angles)[:, None, :] + rotated * jnp.sin(angles)[:, None, :]
    return result.reshape(tok_rows, num_heads * head_size).astype(jnp.bfloat16)

def attend_all(queries, key_rows, values, num_heads, kv_heads, head_size):
    tokens_all = queries.shape[0]
    block_len = math.gcd(tokens_all, 512)
    groups = num_heads // kv_heads
    k_heads = key_rows.astype(jnp.float32).reshape(tokens_all, kv_heads, head_size)
    v_heads = values.astype(jnp.float32).reshape(tokens_all, kv_heads, head_size)

    def one_block(q_block):
        q_heads = q_block.astype(jnp.float32).reshape(block_len, kv_heads, groups, head_size)
        scores = jnp.einsum('tkgd,pkd->kgtp', q_heads, k_heads) * head_size ** (-0.5)
        row_max = lax.optimization_barrier(jnp.max(scores, axis=-1, keepdims=True))
        exp_scores = jnp.exp(scores - row_max)
        rounded = lax.optimization_barrier(exp_scores.astype(jnp.bfloat16)).astype(jnp.float32)
        blended = jnp.einsum('kgtp,pkd->kgtd', rounded, v_heads) / lax.optimization_barrier(jnp.sum(exp_scores, axis=-1))[..., None]
        return blended.transpose(2, 0, 1, 3).reshape(block_len, num_heads * head_size).astype(jnp.bfloat16)
    blocks = queries.reshape(tokens_all // block_len, block_len, num_heads * head_size)
    return lax.map(one_block, blocks).reshape(tokens_all, num_heads * head_size)

def normalize(mixed_rows, gain):
    scale = lax.rsqrt(lax.optimization_barrier(jnp.mean(mixed_rows * mixed_rows, axis=-1, keepdims=True)) + epsilon)
    return (mixed_rows * scale * gain).astype(jnp.bfloat16)

def reference(query_a, key_a, value_a, query_b, key_b, value_b, gain_a, gain_b, out_a, out_b, residual, norm_gain, gate_weight, up_weight, down_weight):
    turned_qa = rotate(query_a, HEADS_A, HEAD_A, 0, gain_a[0])
    turned_ka = rotate(key_a, KV_A, HEAD_A, 0, gain_a[1])
    turned_qb = rotate(query_b, HEADS_B, HEAD_B, 0, gain_b[0])
    turned_kb = rotate(key_b, KV_B, HEAD_B, 0, gain_b[1])
    attn_a = attend_all(turned_qa, turned_ka, value_a, HEADS_A, KV_A, HEAD_A)
    attn_b = attend_all(turned_qb, turned_kb, value_b, HEADS_B, KV_B, HEAD_B)
    cols_a = HEADS_A * HEAD_A // N_TP
    cols_b = HEADS_B * HEAD_B // N_TP
    head_sum = jnp.zeros((TOKENS, D), jnp.float32)
    for block_num in range(N_TP):
        part_a = jnp.dot(attn_a[:, block_num * cols_a:(block_num + 1) * cols_a], out_a[block_num * cols_a:(block_num + 1) * cols_a], preferred_element_type=jnp.float32)
        part_b = jnp.dot(attn_b[:, block_num * cols_b:(block_num + 1) * cols_b], out_b[block_num * cols_b:(block_num + 1) * cols_b], preferred_element_type=jnp.float32)
        head_sum = head_sum + lax.optimization_barrier((part_a + part_b).astype(jnp.bfloat16)).astype(jnp.float32)
    mixed_rows = residual.astype(jnp.float32) + head_sum
    normed = normalize(mixed_rows, norm_gain)
    gate_act = jnp.dot(normed, gate_weight, preferred_element_type=jnp.float32)
    up_act = jnp.dot(normed, up_weight, preferred_element_type=jnp.float32)
    hidden = (jax.nn.silu(gate_act) * up_act).astype(jnp.bfloat16)
    unit_block = FF // N_TP
    branch_sum = jnp.zeros((TOKENS, D), jnp.float32)
    for block_num in range(N_TP):
        part_down = jnp.dot(hidden[:, block_num * unit_block:(block_num + 1) * unit_block], down_weight[block_num * unit_block:(block_num + 1) * unit_block], preferred_element_type=jnp.float32)
        branch_sum = branch_sum + lax.optimization_barrier(part_down.astype(jnp.bfloat16)).astype(jnp.float32)
    return (mixed_rows + 0.5 * branch_sum).astype(jnp.bfloat16)
```

```python
import functools

import jax
import jax.numpy as jnp
import numpy as np
from jax import lax
from jax.experimental import pallas as pl
from jax.experimental.pallas import tpu as pltpu
from jax.sharding import Mesh
from jax.sharding import PartitionSpec as P

HEAD_A = 128
HEAD_B = 64
GRID_W = 64
LANES = 128

epsilon = 1e-06
theta_base = 10000.0


vmem = pl.BlockSpec(memory_space=pltpu.VMEM)


def fetch(value, axis, k):
    n = lax.axis_size(axis)
    return lax.ppermute(value, axis, [((i + k) % n, i) for i in range(n)])


def send(value, axis, k):
    return fetch(value, axis, -k)


def after(value, *others):
    return lax.optimization_barrier((value, *others))[0]


def angle_tables(grid_rows):
    def both(count, head):
        quarter = head // 4
        lane = np.arange(LANES) % head
        inv_freq = (theta_base ** (-4.0 * np.arange(quarter) / head)).astype(np.float32)
        angle = np.arange(count, dtype=np.float32)[:, None] * inv_freq[lane % quarter][None]
        angle = angle.astype(np.float32).astype(np.float64)
        sign = np.where((lane // quarter) % 2 == 0, -1.0, 1.0)
        return np.cos(angle).astype(np.float32), (np.sin(angle) * sign).astype(np.float32)

    rows = np.stack([*both(grid_rows, HEAD_A), *both(grid_rows, HEAD_B)], axis=1)
    cols = np.stack([*both(GRID_W, HEAD_A), *both(GRID_W, HEAD_B)], axis=0)
    return rows, cols


def prep_kernel(blocks, qa, ka, va, qb, kb, vb, ga, gb, rows, cols, q_out, kv_out):
    lane = lax.broadcasted_iota(jnp.int32, (GRID_W, LANES), 1)
    gain_b = [jnp.concatenate([gb[r : r + 1, :]] * 2, axis=1) for r in range(2)]

    def turned(v, gain, cos, sin, head):
        q = head // 4
        if head == LANES:
            mean = jnp.mean(v * v, axis=-1, keepdims=True)
        else:
            sq = v * v
            low = jnp.sum(jnp.where(lane < head, sq, 0.0), axis=-1, keepdims=True)
            high = jnp.sum(jnp.where(lane < head, 0.0, sq), axis=-1, keepdims=True)
            mean = jnp.where(lane < head, low, high) * (1.0 / head)
        v = v * lax.rsqrt(mean + epsilon) * gain
        up = pltpu.roll(v, LANES - q, 1)
        down = pltpu.roll(v, q, 1)
        other = jnp.where((lane // q) % 2 == 0, up, down)
        return v * cos + other * sin

    n_tok = qa.shape[0]
    step = n_tok // blocks

    def put(at, col, value):
        for first in range(0, GRID_W, 8):
            tok = at + first
            block, inside = tok // step, tok % step
            row = (block % 2) * (n_tok // 2) + (block // 2) * step + inside
            q_out[row : row + 8, col : col + LANES] = value[first : first + 8].astype(jnp.bfloat16)

    for r in range(n_tok // GRID_W):
        at = r * GRID_W
        span = slice(at, at + GRID_W)
        tab = []
        for k in range(4):
            head = HEAD_A if k < 2 else HEAD_B
            row = jnp.broadcast_to(rows[k, r : r + 1, :], (GRID_W, LANES))
            tab.append(jnp.where(lane % head < head // 2, row, cols[k]))
        k_a = turned(ka[span, :].astype(jnp.float32), ga[1:2, :], tab[0], tab[1], HEAD_A)
        kv_out[span, 0:128] = k_a.astype(jnp.bfloat16)
        kv_out[span, 128:256] = va[span, :]
        pair = jnp.concatenate(
            [kb[span, :].astype(jnp.float32), vb[span, :].astype(jnp.float32)], axis=1
        )
        k_b = turned(pair, gain_b[1], tab[2], tab[3], HEAD_B)
        kv_out[span, 256:384] = jnp.where(lane < HEAD_B, k_b, pair).astype(jnp.bfloat16)
        for h in range(2):
            part = qa[span, h * LANES : (h + 1) * LANES].astype(jnp.float32)
            put(at, h * LANES, turned(part, ga[0:1, :], tab[0], tab[1], HEAD_A))
        for h in range(2):
            part = qb[span, h * LANES : (h + 1) * LANES].astype(jnp.float32)
            put(at, 256 + h * LANES, turned(part, gain_b[0], tab[2], tab[3], HEAD_B))


def prep(qa, ka, va, qb, kb, vb, ga, gb, rows, cols, blocks):
    n = qa.shape[0]
    return pl.pallas_call(
        functools.partial(prep_kernel, blocks),
        name="prep",
        out_shape=(
            jax.ShapeDtypeStruct((n, 512), jnp.bfloat16),
            jax.ShapeDtypeStruct((n, 384), jnp.bfloat16),
        ),
        in_specs=[vmem] * 10,
        out_specs=(vmem, vmem),
    )(qa, ka, va, qb, kb, vb, ga, gb, rows, cols)


def dot_t(a, b):
    return lax.dot_general(a, b, (((1,), (1,)), ((), ())), preferred_element_type=jnp.float32)


def attend_kernel(n_q, n_kv, *refs):
    q_refs, kv_refs = refs[:n_q], refs[n_q : n_q + n_kv]
    out, q_all, k_a, v_a, k_b, v_b = refs[n_q + n_kv :]
    for b, ref in enumerate(q_refs):
        q_all[b] = ref[...]
    at = 0
    for ref in kv_refs:
        rows = ref.shape[0]
        span = slice(at, at + rows)
        k_a[span, :] = ref[:, 0:128]
        v_a[span, :] = ref[:, 128:256]
        pair = ref[:, 256:384].astype(jnp.float32)
        lane = lax.broadcasted_iota(jnp.int32, pair.shape, 1)
        swap = pltpu.roll(pair, HEAD_B, 1)
        zero = jnp.zeros_like(pair)
        k_b[0, span, :] = jnp.where(lane < HEAD_B, pair, zero).astype(jnp.bfloat16)
        k_b[1, span, :] = jnp.where(lane < HEAD_B, zero, swap).astype(jnp.bfloat16)
        v_b[0, span, :] = jnp.where(lane < HEAD_B, swap, zero).astype(jnp.bfloat16)
        v_b[1, span, :] = jnp.where(lane < HEAD_B, zero, pair).astype(jnp.bfloat16)
        at += rows

    def weights(q, keys, scale):
        s = dot_t(q, keys)
        top = jnp.max(s, axis=-1, keepdims=True)
        p = jnp.exp2((s - top) * (scale * 1.4426950408889634))
        total = jnp.sum(p, axis=-1, keepdims=True)
        return p.astype(jnp.bfloat16), total, top * scale + jnp.log(total)

    scale_a, scale_b = HEAD_A ** (-0.5), HEAD_B ** (-0.5)
    rows = q_all.shape[1]

    def one_block(b, carry):
        q = q_all.at[b]
        lane = lax.broadcasted_iota(jnp.int32, (rows, LANES), 1)
        stats = jnp.zeros((rows, LANES), jnp.float32)
        for h in range(2):
            p, total, lse = weights(q[:, h * 128 : (h + 1) * 128], k_a[...], scale_a)
            o = jnp.dot(p, v_a[...], preferred_element_type=jnp.float32)
            out[b, :, h * 128 : (h + 1) * 128] = (o / total).astype(jnp.bfloat16)
            stats = jnp.where(lane == h, lse, stats)
        for h in range(2):
            cols = slice(256 + h * 128, 256 + (h + 1) * 128)
            p0, t0, l0 = weights(q[:, cols], k_b[0], scale_b)
            p1, t1, l1 = weights(q[:, cols], k_b[1], scale_b)
            o = jnp.dot(p0, v_b[0], preferred_element_type=jnp.float32)
            o += jnp.dot(p1, v_b[1], preferred_element_type=jnp.float32)
            out[b, :, cols] = (o / jnp.where(lane < HEAD_B, t0, t1)).astype(jnp.bfloat16)
            stats = jnp.where(lane == 2 + 2 * h, l0, stats)
            stats = jnp.where(lane == 3 + 2 * h, l1, stats)
        high = stats.astype(jnp.bfloat16).astype(jnp.float32)
        mid = (stats - high).astype(jnp.bfloat16).astype(jnp.float32)
        low = stats - high - mid
        packed = high + pltpu.roll(mid, 8, 1) + pltpu.roll(low, 16, 1)
        out[b, :, 512:640] = packed.astype(jnp.bfloat16)
        return carry

    lax.fori_loop(0, n_q, one_block, 0)


def attend(qs, kvs):
    n = sum(kv.shape[0] for kv in kvs)
    rows = qs[0].shape[0]
    return pl.pallas_call(
        functools.partial(attend_kernel, len(qs), len(kvs)),
        name="attend",
        out_shape=jax.ShapeDtypeStruct((len(qs), rows, 640), jnp.bfloat16),
        in_specs=[vmem] * (len(qs) + len(kvs)),
        out_specs=vmem,
        scratch_shapes=[
            pltpu.VMEM((len(qs), rows, 512), jnp.bfloat16),
            pltpu.VMEM((n, 128), jnp.bfloat16),
            pltpu.VMEM((n, 128), jnp.bfloat16),
            pltpu.VMEM((2, n, 128), jnp.bfloat16),
            pltpu.VMEM((2, n, 128), jnp.bfloat16),
        ],
        compiler_params=pltpu.CompilerParams(vmem_limit_bytes=56 * 1024 * 1024),
    )(*qs, *kvs)


def merge_kernel(*refs):
    parts, out = refs[:-1], refs[-1]
    rows = out.shape[0]
    lane = lax.broadcasted_iota(jnp.int32, (rows, LANES), 1)
    lses = []
    for ref in parts:
        packed = ref[:, 512:640].astype(jnp.float32)
        lses.append(packed + pltpu.roll(packed, LANES - 8, 1) + pltpu.roll(packed, LANES - 16, 1))
    top = functools.reduce(jnp.maximum, lses)
    scales = [jnp.exp(v - top) for v in lses]
    total = functools.reduce(jnp.add, scales)
    scales = [v / total for v in scales]
    for col in range(4):
        acc = jnp.zeros((rows, LANES), jnp.float32)
        for ref, w in zip(parts, scales):
            if col < 2:
                factor = w[:, col : col + 1]
            else:
                first = 2 + 2 * (col - 2)
                factor = jnp.where(
                    lane < HEAD_B, w[:, first : first + 1], w[:, first + 1 : first + 2]
                )
            acc += ref[:, col * 128 : (col + 1) * 128].astype(jnp.float32) * factor
        out[:, col * 128 : (col + 1) * 128] = acc.astype(jnp.bfloat16)


def merge(parts):
    return pl.pallas_call(
        merge_kernel,
        name="merge",
        out_shape=jax.ShapeDtypeStruct((parts[0].shape[0], 512), jnp.bfloat16),
        in_specs=[vmem] * len(parts),
        out_specs=vmem,
    )(*parts)


def normalize(mixed_rows, gain):
    scale = lax.rsqrt(jnp.mean(mixed_rows * mixed_rows, axis=-1, keepdims=True) + epsilon)
    return (mixed_rows * scale * gain).astype(jnp.bfloat16)


def ring_gather(own):
    half = own.shape[0] // 2
    blocks, fwd, bwd = [own], own, own
    for _ in range(3):
        fwd, bwd = fetch(fwd, "z", -1), fetch(bwd, "z", 1)
        blocks += [fwd, bwd]
    blocks += [fetch(fwd[:half], "z", -1), fetch(bwd[half:], "z", 1)]
    return blocks


SHIFTS = (1, 3, 2)


def fetch_all(value, axis):
    got = {k: fetch(value, axis, k) for k in SHIFTS}
    return [value, got[1], got[2], got[3]]


def give_all(parts, axis):
    got = {k: send(parts[k], axis, k) for k in SHIFTS}
    return [parts[0], got[1], got[2], got[3]]


def add_up(parts):
    return functools.reduce(jnp.add, [p.astype(jnp.float32) for p in parts])


def on_device(
    query_a,
    key_a,
    value_a,
    query_b,
    key_b,
    value_b,
    gain_a,
    gain_b,
    out_a,
    out_b,
    residual,
    norm_gain,
    gate_weight,
    up_weight,
    down_weight,
):
    n_tok, width = residual.shape
    at_z, at_y, at_x, at_c = (lax.axis_index(a) for a in ("z", "y", "x", "c"))
    grid_rows = n_tok // GRID_W
    row_tab, col_tab = angle_tables(32 * grid_rows)
    row_tab = row_tab.reshape(32, grid_rows, 4, LANES).transpose(0, 2, 1, 3)
    rows = lax.dynamic_index_in_dim(jnp.asarray(row_tab), at_z * 4 + at_y, 0, keepdims=False)
    queries, kv = prep(
        query_a, key_a, value_a, query_b, key_b, value_b, gain_a, gain_b, rows, jnp.asarray(col_tab), 8
    )
    kvs = ring_gather(kv)
    qs = fetch_all(queries, "y")

    units = gate_weight.shape[1] // 4
    deep = gate_weight.shape[0]
    halves = jnp.stack([gate_weight.reshape(deep, 4, units), up_weight.reshape(deep, 4, units)], 2)
    halves = halves.reshape(deep, 4, 2 * units).transpose(1, 0, 2)
    downs = down_weight.reshape(4, 3, units // 3, LANES).transpose(0, 2, 1, 3)
    downs = downs.reshape(4, units // 3, 3 * LANES)
    quarters = jnp.concatenate([halves, downs], axis=1)
    quarters = jnp.concatenate([quarters, quarters], axis=0)
    quarters = lax.dynamic_slice_in_dim(quarters, at_y, 4, 0)
    mine = give_all([quarters[k] for k in range(4)], "y")
    mine = jnp.stack([mine[(4 - k) % 4] for k in range(4)] * 2)
    mine = lax.dynamic_slice_in_dim(mine, (4 - at_y) % 4, 4, 0)
    out_own = jnp.concatenate([out_a, out_b], axis=0)
    out_other = fetch(out_own, "c", 1)

    mine = after(mine, kvs[-1], kvs[-2])
    gate_up = lax.all_gather(mine[:, :deep], "z", axis=0, tiled=True).reshape(-1, 2 * units)
    down = lax.all_gather(mine[:, deep:], "z", axis=0, tiled=True)
    gate_up_other = fetch(gate_up, "c", 1)
    down = down.reshape(32, units // 3, 3, LANES).transpose(2, 1, 0, 3).reshape(units, width)
    down_other = fetch(down, "c", 1)

    part = attend(qs, kvs)
    attn = merge(give_all([part[k] for k in range(4)], "y"))
    half = n_tok // 2
    attn_own = lax.dynamic_slice_in_dim(attn, at_c * half, half, 0)
    attn_other = fetch(lax.dynamic_slice_in_dim(attn, (1 - at_c) * half, half, 0), "c", 1)
    partial = jnp.dot(attn_own, out_own, preferred_element_type=jnp.float32)
    partial += jnp.dot(attn_other, out_other, preferred_element_type=jnp.float32)
    partial = partial.astype(jnp.bfloat16).reshape(4, half // 4, width)
    partial = jnp.concatenate([partial, partial], axis=0)
    partial = lax.dynamic_slice_in_dim(partial, at_x, 4, 0)
    head_sum = add_up(give_all([partial[k] for k in range(4)], "x"))

    own_rows = n_tok // 8
    own_start = (at_x * 2 + at_c) * own_rows
    own_resid = lax.dynamic_slice_in_dim(residual, own_start, own_rows, 0)
    mixed = own_resid.astype(jnp.float32) + head_sum
    normed = normalize(mixed, norm_gain)

    mid = width // 2
    left = jnp.stack(fetch_all(normed[:, :mid], "y"))
    right = jnp.stack(fetch_all(normed[:, mid:], "x"))
    left = jnp.stack(fetch_all(left, "x"), 1).reshape(16 * own_rows, mid)
    right = jnp.stack(fetch_all(right, "y"), 0).reshape(16 * own_rows, mid)

    def branch(gate_up, down):
        act = jnp.dot(left, gate_up[:mid], preferred_element_type=jnp.float32)
        act += jnp.dot(right, gate_up[mid:], preferred_element_type=jnp.float32)
        hidden = (jax.nn.silu(act[:, :units]) * act[:, units:]).astype(jnp.bfloat16)
        return jnp.dot(hidden, down, preferred_element_type=jnp.float32)

    out = (branch(gate_up, down) + branch(gate_up_other, down_other)).astype(jnp.bfloat16)
    out = out.reshape(4, 4, own_rows, width)
    left = add_up(give_all([out[:, k, :, :mid] for k in range(4)], "x")).astype(jnp.bfloat16)
    right = add_up(give_all([out[k, :, :, mid:] for k in range(4)], "y")).astype(jnp.bfloat16)
    left = add_up(give_all([left[k] for k in range(4)], "y"))
    right = add_up(give_all([right[k] for k in range(4)], "x"))
    branch_sum = jnp.concatenate([left, right], axis=1)
    return (mixed + 0.5 * branch_sum).astype(jnp.bfloat16)


def solution(mesh):
    fine = Mesh(mesh.devices.reshape(8, 4, 4, 2), ("z", "y", "x", "c"))
    sp, tp = ("z", "y"), ("x", "c")
    return jax.shard_map(
        on_device,
        mesh=fine,
        in_specs=(
            P(sp, tp),
            P(sp, tp),
            P(sp, tp),
            P(sp, tp),
            P(sp, tp),
            P(sp, tp),
            P(),
            P(),
            P(tp, None),
            P(tp, None),
            P(sp, None),
            P(),
            P(sp, tp),
            P(sp, tp),
            P(tp, sp),
        ),
        out_specs=P((*sp, *tp), None),
        check_vma=False,
    )
```
